32 devices in a mesh: sp: 8 (over z, y), tp: 4 (over x, core).
Axes of the slice: x: 2, y: 2, z: 4, core: 2. Of those that a mesh axis runs over, the one named last changes fastest.
Arguments:
- mixer_out: bfloat16 [1024, 2048], P('sp'), may hold values from -6 to 6
- conv_out: bfloat16 [1024, 2048], P('sp', 'tp'), may hold values from -350 to 350
- out_cot: bfloat16 [1024, 2048], P('sp'), may hold values from -6 to 6
- routes: int32 [1024, 2], P('sp'), may hold values from 0 to 7, all different within a row; in each aligned block of 128 rows (0 to 127, 128 to 255, ...) at most 64 rows name the same one
- route_weight: float32 [1024, 2], P('sp'), may hold values from 0.3 to 2.5
- gate_weight: bfloat16 [8, 2048, 1024], P('sp', None, 'tp'), may hold values from -0.125 to 0.125
- up_weight: bfloat16 [8, 2048, 1024], P('sp', None, 'tp'), may hold values from -0.125 to 0.125
- down_weight: bfloat16 [8, 1024, 2048], P('sp', 'tp'), may hold values from -0.1875 to 0.1875
- out_weight: bfloat16 [2048, 2048], P('tp'), may hold values from -0.125 to 0.125
- norm_gain: float32 [2048], P('tp'), may hold values from 0.1 to 1.9
- conv_taps: float32 [31, 2048], P(None, 'tp'), may hold values from -1 to 1
Outputs:
- gate_grad: bfloat16 [8, 2048, 1024], P('sp', None, 'tp')
- up_grad: bfloat16 [8, 2048, 1024], P('sp', None, 'tp')
- down_grad: bfloat16 [8, 1024, 2048], P('sp', 'tp')
- proj_grad: float32 [2048, 2048], P('sp', 'tp')
- gated_grad: float32 [1024, 2048], P('sp', 'tp')
The draws below stay inside these ranges and needn't reach their ends.
Inputs may be any that keep to these rules, and one draw needn't show every extreme that they name: `routes`: each row names 2 different experts. Among the rows of one device no expert is named by more than 64 rows, and in every draw some expert is named by exactly 64 rows of some device.
All inputs are finite; a program needn't handle non-finite values.
Results may differ from the reference program's by a relative error of at most 0.0095.
Values may be sent and summed in bfloat16 or wider, within the bound.
A program may use at most 64 MiB of HBM per device.

```python
import math
import jax
import jax.numpy as jnp
import numpy as np
from jax import lax

D = 2048
FE = 1024
KW = 31
TOP = 2
TOK_DEV = 128
TOKENS = 1024
EXPERTS = 8
CAP = 64
N_SP = 8
N_TP = 4


def draw_conv_out(key, part):
    keys = jax.random.split(key, 3)
    column = jnp.exp(jnp.log(3.0) * jnp.arange(D, dtype=jnp.float32) / (D - 1))
    column = column * jnp.exp(jax.random.uniform(keys[2], (1, D), jnp.float32, -0.35, 0.35))
    base = jnp.clip(jax.random.normal(keys[0], (TOKENS, D), jnp.float32), -5.0, 5.0)
    row_scale = jnp.exp(jax.random.uniform(keys[1], (TOKENS, 1), jnp.float32) * jnp.log(10.0))
    return (base * row_scale * column).astype(jnp.bfloat16)


def strengthened(drawn, rng, source, target, blocks, factor):
    owner, partner = [(jnp.arange(drawn.shape[dim]) // (drawn.shape[dim] // blocks)).reshape([-1 if axis == dim else 1 for axis in range(drawn.ndim)]) for dim in (source, target)]
    chosen = jax.random.permutation(rng, blocks)[partner]
    strong = (owner == chosen) | (owner == (partner + blocks // 2) % blocks)
    return jnp.where(strong, factor * drawn, drawn)


def levels(stream_key, extent, pieces, smallest, largest):
    def one(dim, blocks):
        steps = jax.random.uniform(jax.random.fold_in(jax.random.fold_in(stream_key, 6), dim), (blocks,), jnp.float32, smallest / len(pieces), largest / len(pieces))
        return jnp.repeat(jnp.exp(steps), extent[dim] // blocks).reshape((-1,) + (1,) * (len(extent) - dim - 1))

    gain = one(*pieces[0])
    for cut in pieces[1:]:
        gain = gain * one(*cut)
    return gain


def deal_out(own_key, own, number, rows, amount, top, limit, skew):
    ranking = jax.random.permutation(own_key, amount)
    packed, usual = portions_of(amount, rows * top, limit, skew, True), portions_of(amount, rows * top, limit, skew, False)
    places = jnp.arange(amount)

    def named(tallies, turn):
        used = int((tallies > 0).sum())
        fixed = max(1, used // 4)
        moved = fixed + (places - fixed + turn * (used - fixed)) % max(1, amount - fixed)
        return jnp.zeros((amount,), jnp.int32).at[ranking[jnp.where(places < fixed, places, moved)]].set(jnp.asarray(tallies, jnp.int32))

    tallies = jnp.where(number % 4 == 0, named(packed, number // 4), named(usual, number - number // 4 - 1))
    mixed = jax.random.permutation(jax.random.fold_in(own, 3), amount)
    giver, taker = mixed[0:amount // 2 * 2:2], mixed[1:amount // 2 * 2:2]
    room = jnp.minimum(tallies[giver] - 1, limit - tallies[taker]) // 2
    room = jnp.where((giver == ranking[0]) | (taker == ranking[0]) | (tallies[taker] == 0), 0, jnp.maximum(room, 0))
    moved = jax.random.randint(jax.random.fold_in(own, 4), (amount // 2,), 0, 1 << 20) % (room + 1)
    tallies = tallies.at[giver].add(-moved).at[taker].add(moved)
    items = jnp.searchsorted(jnp.cumsum(tallies), jnp.arange(rows * top), side="right").astype(jnp.int32)
    listing = items.reshape(top, rows).T
    listing = listing[jax.random.permutation(jax.random.fold_in(own, 1), rows)]
    turn = jax.random.randint(jax.random.fold_in(own, 2), (rows, 1), 0, top)
    return jnp.take_along_axis(listing, (jnp.arange(top)[None, :] + turn) % top, axis=1)


def portions_of(number_of, total, most, skew, full):
    weights = [(1 << 20) // math.isqrt(grade ** skew) + 1 for grade in range(1, number_of + 1)]
    largest = most if full else min(most, max(-(-total // number_of), total * weights[0] // sum(weights)))
    least = 1 if total - largest >= number_of - 1 else 0
    given, surplus = [largest] + [least] * (number_of - 1), total - largest - least * (number_of - 1)
    while surplus > 0:
        free = [i for i in range(1, number_of) if given[i] < largest] or [i for i in range(1, number_of) if given[i] < most]
        pool, left = sum([weights[i] for i in free]), surplus
        for i in free:
            more = min(most - given[i], max(1, left * weights[i] // pool), surplus)
            given[i] = given[i] + more
            surplus = surplus - more
    return np.array(given)


def centred(stream_key, shape, deviation, most, pieces=(), held_as=jnp.bfloat16):
    values = deviation * jax.random.normal(stream_key, shape, jnp.float32)
    if pieces:
        values = values * levels(stream_key, shape, pieces, -0.22, 0.18)
    return jnp.clip(values, -most, most).astype(held_as)


def noise_with(stream_key, shape, deviation, most, pieces, heavy, kind=jnp.bfloat16):
    array = deviation * jax.random.normal(stream_key, shape, jnp.float32)
    if pieces:
        array = array * levels(stream_key, shape, pieces, -0.22, 0.18)
    return jnp.clip(strengthened(array, jax.random.fold_in(stream_key, 3), *heavy), -most, most).astype(kind)


def setup_inputs(seed: int = 0) -> dict:
    arg_keys = jax.random.split(jax.random.key(seed), 12)
    mixer_out = centred(arg_keys[0], (TOKENS, D), 1.0, 6.0, ((0, 8),))
    conv_out = draw_conv_out(jax.random.fold_in(arg_keys[11], 71), 0)
    out_cot = noise_with(arg_keys[2], (TOKENS, D), 1.0, 6.0, ((0, 8),), (0, 1, 8, 2.0))
    routes_keys = jax.random.split(jax.random.fold_in(arg_keys[3], 1), TOKENS // TOK_DEV)
    routes_turns = jax.random.permutation(jax.random.fold_in(arg_keys[3], 3), TOKENS // TOK_DEV)
    routes = jax.vmap(lambda own, number: deal_out(jax.random.fold_in(arg_keys[3], 2), own, number, TOK_DEV, EXPERTS, TOP, CAP, 2))(routes_keys, routes_turns).reshape((TOKENS, TOP))
    route_weight = jnp.clip(jnp.exp(math.log(2.5) - 2.1202635 * jax.random.uniform(arg_keys[4], (TOKENS, TOP), jnp.float32) ** levels(arg_keys[4], (TOKENS, TOP), ((0, 8),), -0.2, 0.2)), 0.3, 2.5)
    gate_weight = centred(arg_keys[5], (EXPERTS, D, FE), D ** -0.5, 0.125, ((0, 8), (2, 4)))
    up_weight = centred(arg_keys[6], (EXPERTS, D, FE), D ** -0.5, 0.125, ((0, 8), (2, 4)))
    down_weight = centred(arg_keys[7], (EXPERTS, FE, D), FE ** -0.5, 0.1875, ((0, 8), (1, 4)))
    out_weight = centred(arg_keys[8], (D, D), D ** -0.5, 0.125, ((0, 4),))
    norm_gain = jnp.clip(1.0 + 0.18 * jax.random.normal(arg_keys[9], (D,), jnp.float32), 0.1, 1.9)
    conv_taps = centred(arg_keys[10], (KW, D), KW ** -0.5, 1.0, ((1, 4),), jnp.float32)
    return {"mixer_out": mixer_out, "conv_out": conv_out, "out_cot": out_cot, "routes": routes, "route_weight": route_weight, "gate_weight": gate_weight, "up_weight": up_weight, "down_weight": down_weight, "out_weight": out_weight, "norm_gain": norm_gain, "conv_taps": conv_taps}


norm_epsilon = 1e-05

def expert_backward(x_rows, cot_rows, w_gate, w_up, w_down, parts):
    pre_gate = jnp.dot(x_rows, w_gate, preferred_element_type=jnp.float32)
    pre_up = jnp.dot(x_rows, w_up, preferred_element_type=jnp.float32)
    sig_gate = jax.nn.sigmoid(pre_gate)
    activation = (pre_gate * sig_gate * pre_up).astype(jnp.bfloat16)
    down_g = lax.dot_general(activation, cot_rows, (((0,), (0,)), ((), ())), preferred_element_type=jnp.float32).astype(jnp.bfloat16)
    act_grad = lax.dot_general(cot_rows, w_down, (((1,), (1,)), ((), ())), preferred_element_type=jnp.float32)
    gate_pre_grad = (act_grad * pre_up * sig_gate * (1.0 + pre_gate * (1.0 - sig_gate))).astype(jnp.bfloat16)
    up_pre_grad = (act_grad * pre_gate * sig_gate).astype(jnp.bfloat16)
    gate_g = lax.dot_general(x_rows, gate_pre_grad, (((0,), (0,)), ((), ())), preferred_element_type=jnp.float32).astype(jnp.bfloat16)
    up_g = lax.dot_general(x_rows, up_pre_grad, (((0,), (0,)), ((), ())), preferred_element_type=jnp.float32).astype(jnp.bfloat16)
    part_width = w_gate.shape[1] // parts
    total_back = jnp.zeros((x_rows.shape[0], w_gate.shape[0]), jnp.float32)
    for part_index in range(parts):
        lower = part_index * part_width
        upper = lower + part_width
        partial_value = lax.dot_general(gate_pre_grad[:, lower:upper], w_gate[:, lower:upper], (((1,), (1,)), ((), ())), preferred_element_type=jnp.float32)
        partial_value = partial_value + lax.dot_general(up_pre_grad[:, lower:upper], w_up[:, lower:upper], (((1,), (1,)), ((), ())), preferred_element_type=jnp.float32)
        rounded = lax.optimization_barrier(partial_value.astype(jnp.bfloat16))
        total_back = total_back + rounded.astype(jnp.float32)
    return (gate_g, up_g, down_g, total_back)

def reference(mixer_out, conv_out, out_cot, routes, route_weight, gate_weight, up_weight, down_weight, out_weight, norm_gain, conv_taps):
    entries = TOKENS * TOP
    flat_routes = routes.reshape(-1).astype(jnp.int32)
    one_hot = (flat_routes[:, None] == jnp.arange(EXPERTS, dtype=jnp.int32)[None, :]).astype(jnp.int32)
    by_source = one_hot.reshape(N_SP, TOK_DEV * TOP, EXPERTS)
    earlier = jnp.cumsum(by_source, axis=1) - by_source
    within = lax.optimization_barrier(jnp.sum(earlier * by_source, axis=2)).reshape(-1)
    source_index = jnp.arange(entries, dtype=jnp.int32) // (TOK_DEV * TOP)
    slot_index = (source_index * CAP + within).astype(jnp.int32)
    table = jnp.full((EXPERTS, N_SP * CAP), entries, jnp.int32)
    table = table.at[flat_routes, slot_index].set(jnp.arange(entries, dtype=jnp.int32))
    weights_flat = route_weight.reshape(-1)

    def per_expert(carry, inputs):
        w_gate, w_up, w_down, entry_ids = inputs
        token_ids = (entry_ids // TOP).astype(jnp.int32)
        x_rows = jnp.take(mixer_out, token_ids, axis=0, mode='fill', fill_value=0)
        cot_rows = jnp.take(out_cot, token_ids, axis=0, mode='fill', fill_value=0)
        scale_rows = jnp.take(weights_flat, entry_ids, axis=0, mode='fill', fill_value=0)
        row_cot = (scale_rows[:, None] * cot_rows.astype(jnp.float32)).astype(jnp.bfloat16)
        gate_g, up_g, down_g, total_back = expert_backward(x_rows, row_cot, w_gate, w_up, w_down, N_TP)
        row_back = lax.optimization_barrier(total_back.astype(jnp.bfloat16))
        carry = carry.at[token_ids].add(row_back.astype(jnp.float32), mode='drop')
        return (carry, (gate_g, up_g, down_g))
    summed, stacked = lax.scan(per_expert, out_cot.astype(jnp.float32), (gate_weight, up_weight, down_weight, table))
    gate_grad, up_grad, down_grad = stacked
    mix_grad = summed.astype(jnp.bfloat16)
    conv_vals = conv_out.astype(jnp.float32)
    inv_rms = lax.rsqrt(lax.optimization_barrier(jnp.mean(conv_vals * conv_vals, axis=1, keepdims=True)) + norm_epsilon)
    normed = conv_vals * inv_rms * norm_gain[None, :]
    sig_norm = jax.nn.sigmoid(normed)
    activated = (normed * sig_norm).astype(jnp.bfloat16)
    proj_grad = lax.dot_general(mix_grad, activated, (((0,), (0,)), ((), ())), preferred_element_type=jnp.float32)
    norm_in_grad = lax.dot_general(mix_grad, out_weight, (((1,), (1,)), ((), ())), preferred_element_type=jnp.float32)
    scaled = norm_in_grad * sig_norm * (1.0 + normed * (1.0 - sig_norm)) * norm_gain[None, :]
    conv_grad = inv_rms * scaled - conv_vals * inv_rms ** 3 * lax.optimization_barrier(jnp.mean(conv_vals * scaled, axis=1, keepdims=True))
    padded = jnp.pad(conv_grad, ((0, KW - 1), (0, 0)))
    gated_grad = jnp.zeros((TOKENS, D), jnp.float32)
    for tap_index in range(KW):
        gated_grad = gated_grad + conv_taps[tap_index][None, :] * padded[tap_index:tap_index + TOKENS]
    return (gate_grad, up_grad, down_grad, proj_grad, gated_grad)
```

```python
import functools

import jax
import jax.numpy as jnp
from jax import lax
from jax.experimental import pallas as pl
from jax.experimental.pallas import tpu as pltpu
from jax.sharding import PartitionSpec as P

norm_epsilon = 1e-05


def shifted(block, axis, distance):
    devices = range(lax.axis_size(axis))
    route = [(i - distance, i) for i in devices if i - distance in devices]
    return lax.ppermute(block, axis, route)


def expert_backward(x_rows, cot_rows, w_gate, w_up, w_down):
    pre_gate = jnp.dot(x_rows, w_gate, preferred_element_type=jnp.float32)
    pre_up = jnp.dot(x_rows, w_up, preferred_element_type=jnp.float32)
    sig_gate = jax.nn.sigmoid(pre_gate)
    activation = (pre_gate * sig_gate * pre_up).astype(jnp.bfloat16)
    down_g = lax.dot_general(
        activation, cot_rows, (((0,), (0,)), ((), ())), preferred_element_type=jnp.float32
    ).astype(jnp.bfloat16)
    act_grad = lax.dot_general(
        cot_rows, w_down, (((1,), (1,)), ((), ())), preferred_element_type=jnp.float32
    )
    gate_pre_grad = (act_grad * pre_up * sig_gate * (1.0 + pre_gate * (1.0 - sig_gate))).astype(
        jnp.bfloat16
    )
    up_pre_grad = (act_grad * pre_gate * sig_gate).astype(jnp.bfloat16)
    gate_g = lax.dot_general(
        x_rows, gate_pre_grad, (((0,), (0,)), ((), ())), preferred_element_type=jnp.float32
    ).astype(jnp.bfloat16)
    up_g = lax.dot_general(
        x_rows, up_pre_grad, (((0,), (0,)), ((), ())), preferred_element_type=jnp.float32
    ).astype(jnp.bfloat16)
    partial_value = lax.dot_general(
        gate_pre_grad, w_gate, (((1,), (1,)), ((), ())), preferred_element_type=jnp.float32
    )
    partial_value = partial_value + lax.dot_general(
        up_pre_grad, w_up, (((1,), (1,)), ((), ())), preferred_element_type=jnp.float32
    )
    rounded = lax.optimization_barrier(partial_value.astype(jnp.bfloat16))
    return (gate_g, up_g, down_g, rounded.astype(jnp.float32))


def on_device(
    mixer_out,
    conv_out,
    out_cot,
    routes,
    route_weight,
    gate_weight,
    up_weight,
    down_weight,
    out_weight,
    norm_gain,
    conv_taps,
):
    tokens_here, model_width = out_cot.shape
    route_count = routes.shape[1]
    experts = lax.axis_size("sp")
    capacity = 2 * tokens_here * route_count // experts
    quarter = conv_out.shape[1]
    first_col = lax.axis_index("tp") * quarter
    flat_routes = routes.reshape(-1)
    one_hot = (flat_routes[:, None] == jnp.arange(experts, dtype=jnp.int32)[None, :]).astype(
        jnp.int32
    )
    within = jnp.sum((jnp.cumsum(one_hot, axis=0) - one_hot) * one_hot, axis=1)
    slot_index = flat_routes * capacity + within
    row_cot = (route_weight[:, :, None] * out_cot[:, None, :].astype(jnp.float32)).astype(
        jnp.bfloat16
    )
    row_cot = row_cot.reshape(tokens_here * route_count, model_width)
    rows_input = jnp.repeat(mixer_out, route_count, axis=0)
    w_gate = gate_weight[0]
    w_up = up_weight[0]
    w_down = down_weight[0]
    rows_part = lax.dynamic_slice_in_dim(rows_input, first_col, quarter, 1)
    cot_part = lax.dynamic_slice_in_dim(row_cot, first_col, quarter, 1)
    send_rows = jnp.zeros((experts * capacity, quarter), jnp.bfloat16).at[slot_index].set(rows_part)
    send_cot = jnp.zeros((experts * capacity, quarter), jnp.bfloat16).at[slot_index].set(cot_part)
    rows_slice, cot_slice = (
        lax.all_to_all(send_rows, "sp", split_axis=0, concat_axis=0, tiled=True),
        lax.all_to_all(send_cot, "sp", split_axis=0, concat_axis=0, tiled=True),
    )
    x_rows, cot_rows = (
        lax.all_gather(rows_slice, "tp", axis=1, tiled=True),
        lax.all_gather(cot_slice, "tp", axis=1, tiled=True),
    )
    gate_g, up_g, down_g, partial_value = expert_backward(x_rows, cot_rows, w_gate, w_up, w_down)
    back_slice = lax.psum_scatter(
        partial_value.astype(jnp.bfloat16), "tp", scatter_dimension=1, tiled=True
    )
    returned = lax.all_to_all(back_slice, "sp", split_axis=0, concat_axis=0, tiled=True)
    picked = returned[slot_index].astype(jnp.float32).reshape(tokens_here, route_count, quarter)
    own_cot = lax.dynamic_slice_in_dim(out_cot, first_col, quarter, 1).astype(jnp.float32)
    mix_part = (own_cot + jnp.sum(picked, axis=1)).astype(jnp.bfloat16)
    mix_grad = lax.all_gather(mix_part, "tp", axis=1, tiled=True)
    conv_vals = conv_out.astype(jnp.float32)
    power_sum = lax.psum(jnp.sum(conv_vals * conv_vals, axis=1), "tp")
    inv_rms = lax.rsqrt(power_sum / model_width + norm_epsilon)[:, None]
    normed = conv_vals * inv_rms * norm_gain[None, :]
    sig_norm = jax.nn.sigmoid(normed)
    activated = (normed * sig_norm).astype(jnp.bfloat16)
    proj_grad = lax.psum_scatter(
        lax.dot_general(
            mix_grad, activated, (((0,), (0,)), ((), ())), preferred_element_type=jnp.float32
        ),
        "sp",
        scatter_dimension=0,
        tiled=True,
    )
    norm_in_grad = lax.dot_general(
        mix_grad, out_weight, (((1,), (1,)), ((), ())), preferred_element_type=jnp.float32
    )
    scaled = norm_in_grad * sig_norm * (1.0 + normed * (1.0 - sig_norm)) * norm_gain[None, :]
    dot_sum = lax.psum(jnp.sum(conv_vals * scaled, axis=1), "tp")
    conv_grad = inv_rms * scaled - conv_vals * inv_rms**3 * (dot_sum / model_width)[:, None]
    reach = conv_taps.shape[0] - 1
    following = shifted(conv_grad[:reach].astype(jnp.bfloat16), "sp", -1).astype(jnp.float32)
    extended = jnp.concatenate([conv_grad, following], axis=0)
    gated_grad = jnp.zeros((tokens_here, quarter), jnp.float32)
    for tap_index in range(reach + 1):
        gated_grad = (
            gated_grad
            + conv_taps[tap_index][None, :] * extended[tap_index : tap_index + tokens_here]
        )
    return (gate_g[None], up_g[None], down_g[None], proj_grad, gated_grad)


VMEM = pl.BlockSpec(memory_space=pltpu.VMEM)
DMA = pltpu.SemaphoreType.DMA
MESH = pl.DeviceIdType.MESH


def greet(peers):
    barrier = pltpu.get_barrier_semaphore()
    for peer in peers:
        pl.semaphore_signal(barrier, inc=1, device_id=peer, device_id_type=MESH)
    pl.semaphore_wait(barrier, len(peers))


def send(src, dst, send_sem, recv_sem, device):
    return pltpu.make_async_remote_copy(
        src_ref=src,
        dst_ref=dst,
        send_sem=send_sem,
        recv_sem=recv_sem,
        device_id=device,
        device_id_type=MESH,
    )


def places():
    me, q = lax.axis_index("sp"), lax.axis_index("tp")
    twin = q + 1 - 2 * (q % 2)
    across = (q + 2) % 4
    return me, q, twin, across


def params(number):
    return pltpu.CompilerParams(collective_id=number, has_side_effects=True)


def span(index, size):
    return pl.ds(pl.multiple_of(index * size, size), size)


def dispatch_kernel(n, s_ref, sq_ref, xc_ref, sqs_ref, own_sem, a_s, a_r, t_s, t_r, x_s, x_r, f_s, f_r, q_s, q_r):
    me, q, twin, across = places()
    rows, cols = s_ref.shape[2], s_ref.shape[3]
    twin_across = (twin + 2) % 4
    greet([((me + j) % n, q) for j in range(1, n)] + [(me, twin), (me, across), (me, twin_across)])
    order = [n // 2] + [j for d in range(1, n // 2) for j in (n // 2 - d, n // 2 + d)]
    pending = []
    for j in order:
        d = (me + j) % n
        c = send(s_ref.at[d], xc_ref.at[:, span(me, rows), span(q, cols)], a_s.at[j], a_r.at[j], (d, q))
        c.start()
        pending.append(c)
    own = pltpu.make_async_copy(s_ref.at[me], xc_ref.at[:, span(me, rows), span(q, cols)], own_sem)
    own.start()
    own_sq = pltpu.make_async_copy(sq_ref, sqs_ref.at[q], q_s.at[3])
    own_sq.start()
    small = []
    for k, peer in enumerate((twin, across, twin_across)):
        c = send(sq_ref, sqs_ref.at[q], q_s.at[k], q_r.at[k], (me, peer))
        c.start()
        small.append(c)

    def block(j, quarter):
        return xc_ref.at[:, span((me + n - j) % n, rows), span(quarter, cols)]

    last = []

    def relay(j):
        arrived = send(block(j, across), block(j, across), x_s.at[j], x_r.at[j], (me, across))
        arrived.wait_recv()
        c = send(block(j, across), block(j, across), f_s.at[j], f_r.at[j], (me, twin))
        c.start()
        last.append(c)
        pending.append(c)

    queue = [0] + order
    for at, j in enumerate(queue):
        if j == 0:
            own.wait()
        else:
            send(s_ref.at[me], block(j, q), a_s.at[j], a_r.at[j], (me, q)).wait_recv()
        c = send(block(j, q), block(j, q), x_s.at[j], x_r.at[j], (me, across))
        c.start()
        pending.append(c)
        c = send(block(j, q), block(j, q), t_s.at[j], t_r.at[j], (me, twin))
        c.start()
        pending.append(c)
        last.append(c)
        if at >= 1:
            relay(queue[at - 1])
    relay(queue[-1])
    for c in last:
        c.wait_recv()
    for c in small:
        c.wait()
    own_sq.wait()
    for c in pending:
        c.wait_send()


def return_kernel(n, p_ref, act_ref, ret_ref, all_ref, d_r, sx, rx, back, d1_s, d1_r, x_s, x_r, a_s, a_r, o_sem,
                  up_s, up_r, dn_s, dn_r, y_s, y_r):
    me, q, twin, across = places()
    rows, cols = ret_ref.shape[0] // n, ret_ref.shape[1]
    tokens = act_ref.shape[0]
    level, side = me // 2, me % 2
    mate = me + 1 - 2 * side
    levels = n // 2
    below, above = (me + n - 2) % n, (me + 2) % n
    greet([((me + j) % n, q) for j in range(1, n)] + [(me, twin), (me, across)])
    twin_across = (twin + 2) % 4
    order = [n // 2] + [j for d in range(1, n // 2) for j in (n // 2 - d, n // 2 + d)] + [0]
    waits = []
    firsts = {}
    for j in order:
        for k, quarter in enumerate((twin, twin_across)):
            part = span((me + j) % n, rows)
            c = send(p_ref.at[part, span(quarter, cols)], d_r.at[k, part], d1_s.at[k, j], d1_r.at[k, j], (me, twin))
            c.start()
            firsts[k, j] = c
            waits.append(c)
    own = pltpu.make_async_copy(act_ref, all_ref.at[span(me, tokens)], o_sem)
    own.start()

    def piece(lvl):
        return all_ref.at[span((lvl + levels) % levels * 2 + side, tokens)]

    def ways(t):
        up = send(act_ref if t == 0 else piece(level - t), piece(level - t), up_s.at[t], up_r.at[t], (above, q))
        dn = send(act_ref if t == 0 else piece(level + t), piece(level + t), dn_s.at[t], dn_r.at[t], (below, q))
        return up, dn

    def over(k, lvl):
        src = act_ref if k == 0 else piece(lvl)
        return send(src, piece(lvl), y_s.at[k], y_r.at[k], (mate, q))

    def start_ways(t):
        up, dn = ways(t)
        pl.when(jnp.logical_and(level - t >= 0, level + 1 < levels))(up.start)
        pl.when(jnp.logical_and(level + t < levels, level >= 1))(dn.start)

    def take(t):
        got_up = send(act_ref, piece(level - 1 - t), up_s.at[t], up_r.at[t], (above, q))
        got_dn = send(act_ref, piece(level + 1 + t), dn_s.at[t], dn_r.at[t], (below, q))

        @pl.when(level - 1 - t >= 0)
        def _():
            got_up.wait_recv()
            over(1 + t, level - 1 - t).start()

        @pl.when(level + 1 + t < levels)
        def _():
            got_dn.wait_recv()
            over(levels + t, level + 1 + t).start()

    start_ways(0)
    over(0, level).start()

    def first(j):
        part = span((me + j) % n, rows)
        for k in range(2):
            firsts[k, j].wait_recv()
        near = p_ref[part, span(across, cols)].astype(jnp.float32) + d_r[1, part].astype(jnp.float32)
        sx[part] = near.astype(jnp.bfloat16)
        c = send(sx.at[part], rx.at[part], x_s.at[j], x_r.at[j], (me, across))
        c.start()
        waits.append(c)
        return c

    outgoing = {}

    def second(j, c):
        part = span((me + j) % n, rows)
        c.wait_recv()
        total = p_ref[part, span(q, cols)].astype(jnp.float32) + d_r[0, part].astype(jnp.float32)
        total = (total + rx[part].astype(jnp.float32)).astype(jnp.bfloat16)
        if j == 0:
            ret_ref[part] = total
        else:
            back[part] = total
            a = send(back.at[part], ret_ref.at[span(me, rows)], a_s.at[j], a_r.at[j], ((me + j) % n, q))
            a.start()
            outgoing[j] = a
            waits.append(a)

    crossing = [first(j) for j in order]
    take(0)
    start_ways(1)
    for at, j in enumerate(order):
        second(j, crossing[at])
        if at == 2:
            take(1)
            start_ways(2)
        if at == 5:
            take(2)
    for j in order[:-1]:
        got = send(back.at[span(me, rows)], ret_ref.at[span((me + n - j) % n, rows)], a_s.at[j], a_r.at[j], (me, q))
        got.wait_recv()
    for c in waits:
        c.wait_send()
    own.wait()

    def other(lvl):
        return all_ref.at[span((lvl + levels) % levels * 2 + 1 - side, tokens)]

    for t in range(levels - 1):
        up, dn = ways(t)
        pl.when(jnp.logical_and(level - t >= 0, level + 1 < levels))(up.wait_send)
        pl.when(jnp.logical_and(level + t < levels, level >= 1))(dn.wait_send)
    for k in range(2 * levels - 1):
        lvl = level - k if k < levels else level + k - levels + 1
        here = lvl >= 0 if k < levels else lvl < levels

        @pl.when(here)
        def _():
            over(k, lvl).wait_send()
            send(act_ref, other(lvl), y_s.at[k], y_r.at[k], (mate, q)).wait_recv()


def tail_kernel(n, mix_ref, act_ref, w_ref, conv_ref, inv_ref, gain_ref, taps_ref, gated_ref, proj_ref,
                mg, pr, ext, halo, dots, m_s, m_r, f_s, f_r, a_s, a_r, o_sem, d_s, d_r, h_s, h_r):
    me, q, twin, across = places()
    twin_across = (twin + 2) % 4
    tokens, cols = mix_ref.shape
    block = proj_ref.shape[0]
    reach = taps_ref.shape[0] - 1
    pad = halo.shape[1]
    greet([((me + j) % n, q) for j in range(1, n)] + [(me, twin), (me, across), (me, twin_across)])
    to_x = send(mix_ref, mg.at[:, span(q, cols)], m_s.at[0], m_r.at[0], (me, across))
    to_x.start()
    to_twin = send(mix_ref, mg.at[:, span(q, cols)], m_s.at[1], m_r.at[1], (me, twin))
    to_twin.start()
    own = pltpu.make_async_copy(mix_ref, mg.at[:, span(q, cols)], o_sem.at[0])
    own.start()
    conv = conv_ref[...].astype(jnp.float32)
    inv = inv_ref[...]
    gain = gain_ref[...]
    normed = conv * inv * gain
    sig = jax.nn.sigmoid(normed)
    slope = sig * (1.0 + normed * (1.0 - sig)) * gain
    to_x.wait_recv()
    relay = send(mg.at[:, span(across, cols)], mg.at[:, span(across, cols)], f_s, f_r, (me, twin))
    relay.start()
    to_twin.wait_recv()
    relay.wait_recv()
    own.wait()
    pending = [to_x, to_twin, relay]
    incoming = []
    order = [n // 2] + [j for d in range(1, n // 2) for j in (n // 2 - d, n // 2 + d)]
    for j in order:
        d = (me + j) % n
        c = send(mg.at[:, span(d, block)], pr.at[span(me, tokens)], a_s.at[j], a_r.at[j], (d, q))
        c.start()
        pending.append(c)
        incoming.append(
            send(mg.at[:, span(d, block)], pr.at[span((me + n - j) % n, tokens)], a_s.at[j], a_r.at[j], (d, q))
        )
    mine = pltpu.make_async_copy(mg.at[:, span(me, block)], pr.at[span(me, tokens)], o_sem.at[1])
    mine.start()
    into = lax.dot_general(mg[...], w_ref[...], (((1,), (1,)), ((), ())), preferred_element_type=jnp.float32)
    scaled = into * slope
    dot = jnp.sum(conv * scaled, axis=1, keepdims=True)
    dots[0] = jnp.broadcast_to(dot, dots.shape[1:])
    small = []
    for k, peer in enumerate((twin, across, twin_across)):
        c = send(dots.at[0], dots.at[k + 1], d_s.at[k], d_r.at[k], (me, peer))
        c.start()
        small.append(c)
    ext[pl.ds(0, tokens)] = inv * scaled
    for c in small:
        c.wait()
    total = dots[0] + dots[1] + dots[2] + dots[3]
    total = total[:, :1]
    grad = ext[pl.ds(0, tokens)] - conv * (inv * inv * inv * (total / (cols * 4)))
    ext[pl.ds(0, tokens)] = grad
    halo[0] = grad[:pad].astype(jnp.bfloat16)
    shift = send(halo.at[0], halo.at[1], h_s, h_r, ((me + n - 1) % n, q))
    pl.when(me > 0)(shift.start)

    mine.wait()
    for c in incoming:
        c.wait_recv()
    proj_ref[...] = lax.dot_general(
        pr[...], act_ref[...], (((0,), (0,)), ((), ())), preferred_element_type=jnp.float32
    )

    @pl.when(me < n - 1)
    def _():
        shift.wait_recv()
        ext[pl.ds(tokens, pad)] = halo[1].astype(jnp.float32)

    @pl.when(me == n - 1)
    def _():
        ext[pl.ds(tokens, pad)] = jnp.zeros((pad, cols), jnp.float32)

    pl.when(me > 0)(shift.wait_send)
    step = 128
    for low in range(0, cols, step):
        band = pl.ds(low, step)
        acc = taps_ref[pl.ds(0, 1), band] * ext[pl.ds(0, tokens), band]
        for tap in range(1, reach + 1):
            acc = acc + taps_ref[pl.ds(tap, 1), band] * ext[pl.ds(tap, tokens), band]
        gated_ref[:, band] = acc
    for c in pending:
        c.wait_send()


def near_plan(mixer_out, conv_out, out_cot, routes, route_weight, gate_weight, up_weight, down_weight, out_weight,
              norm_gain, conv_taps):
    tokens_here, model_width = out_cot.shape
    n = lax.axis_size("sp")
    capacity = 2 * tokens_here * routes.shape[1] // n
    quarter = conv_out.shape[1]
    first_col = lax.axis_index("tp") * quarter
    bf16, f32 = jnp.bfloat16, jnp.float32
    experts = jnp.arange(n, dtype=jnp.int32)[:, None, None]
    named = routes.T[None] == experts
    member = jnp.any(named, axis=1)
    weight_of = jnp.sum(jnp.where(named, route_weight.T[None], 0.0), axis=1)
    earlier = jnp.arange(tokens_here)[:, None] < jnp.arange(tokens_here)[None, :]
    rank = jnp.dot(member.astype(bf16), earlier.astype(bf16), preferred_element_type=f32).astype(jnp.int32)
    chosen = (rank[:, None, :] == jnp.arange(capacity)[None, :, None]) & member[:, None, :]
    select = chosen.astype(bf16).reshape(n * capacity, tokens_here)
    slot_weight = jnp.sum(jnp.where(chosen, weight_of[:, None, :], 0.0), axis=2)
    own_x = lax.dynamic_slice_in_dim(mixer_out, first_col, quarter, 1)
    own_cot = lax.dynamic_slice_in_dim(out_cot, first_col, quarter, 1)
    rows = jnp.dot(select, own_x, preferred_element_type=f32).astype(bf16)
    cots = jnp.dot(select, own_cot, preferred_element_type=f32) * slot_weight.reshape(-1, 1)
    packed = jnp.stack(
        [rows.reshape(n, capacity, quarter), cots.astype(bf16).reshape(n, capacity, quarter)], axis=1
    )
    conv_vals = conv_out.astype(f32)
    squares = jnp.sum(conv_vals * conv_vals, axis=1)
    squares = jnp.broadcast_to(squares[None, :], (8, tokens_here))
    total_rows = n * capacity
    shape = jax.ShapeDtypeStruct
    x_and_cot, all_squares = pl.pallas_call(
        functools.partial(dispatch_kernel, n),
        out_shape=(shape((2, total_rows, model_width), bf16), shape((4, 8, tokens_here), f32)),
        in_specs=[VMEM] * 2,
        out_specs=(VMEM, VMEM),
        scratch_shapes=[DMA] + [DMA((n,))] * 8 + [DMA((4,))] * 2,
        compiler_params=params(0),
        name="dispatch",
    )(packed, squares)
    inv_rms = lax.rsqrt(jnp.sum(all_squares[:, 0], axis=0) / model_width + norm_epsilon)[:, None]
    normed = conv_vals * inv_rms * norm_gain[None, :]
    activated = (normed * jax.nn.sigmoid(normed)).astype(bf16)
    gate_g, up_g, down_g, partial_value = expert_backward(
        x_and_cot[0], x_and_cot[1], gate_weight[0], up_weight[0], down_weight[0]
    )
    levels = n // 2
    returned, act_all = pl.pallas_call(
        functools.partial(return_kernel, n),
        out_shape=(shape((total_rows, quarter), bf16), shape((n * tokens_here, quarter), bf16)),
        in_specs=[VMEM] * 2,
        out_specs=(VMEM, VMEM),
        scratch_shapes=[pltpu.VMEM((2, total_rows, quarter), bf16)]
        + [pltpu.VMEM((total_rows, quarter), bf16)] * 3
        + [DMA((2, n))] * 2
        + [DMA((n,))] * 4
        + [DMA]
        + [DMA((levels,))] * 4
        + [DMA((2 * levels,))] * 2,
        compiler_params=params(1),
        name="give_back",
    )(partial_value.astype(bf16), activated)
    summed = lax.dot_general(select, returned, (((0,), (0,)), ((), ())), preferred_element_type=f32)
    mix_part = (own_cot.astype(f32) + summed).astype(bf16)
    pad = -(-(conv_taps.shape[0] - 1) // 16) * 16
    gated_grad, proj_grad = pl.pallas_call(
        functools.partial(tail_kernel, n),
        out_shape=(shape((tokens_here, quarter), f32), shape((model_width // n, quarter), f32)),
        in_specs=[VMEM] * 7,
        out_specs=(VMEM, VMEM),
        scratch_shapes=[
            pltpu.VMEM((tokens_here, model_width), bf16),
            pltpu.VMEM((n * tokens_here, model_width // n), bf16),
            pltpu.VMEM((tokens_here + pad, quarter), f32),
            pltpu.VMEM((2, pad, quarter), bf16),
            pltpu.VMEM((4, tokens_here, 128), f32),
            DMA((2,)), DMA((2,)), DMA, DMA, DMA((n,)), DMA((n,)), DMA((2,)), DMA((3,)), DMA((3,)), DMA, DMA,
        ],
        compiler_params=params(2),
        name="tail",
    )(mix_part, act_all, out_weight, conv_out, inv_rms, norm_gain[None, :], conv_taps)
    return (gate_g[None], up_g[None], down_g[None], proj_grad, gated_grad)


def either_plan(*arrays):
    near = lax.axis_size("tp") == 4 and lax.axis_size("sp") in (4, 8)
    return near_plan(*arrays) if near else on_device(*arrays)


def solution(mesh):
    placed = (
        P("sp", None),
        P("sp", "tp"),
        P("sp", None),
        P("sp", None),
        P("sp", None),
        P("sp", None, "tp"),
        P("sp", None, "tp"),
        P("sp", "tp", None),
        P("tp", None),
        P("tp"),
        P(None, "tp"),
    )
    return jax.shard_map(
        either_plan,
        mesh=mesh,
        in_specs=placed,
        out_specs=(
            P("sp", None, "tp"),
            P("sp", None, "tp"),
            P("sp", "tp", None),
            P("sp", "tp"),
            P("sp", "tp"),
        ),
        check_vma=False,
    )
```

```python
import functools

import jax
import jax.numpy as jnp
from jax import lax
from jax.experimental import pallas as pl
from jax.experimental.pallas import tpu as pltpu
from jax.sharding import PartitionSpec as P

norm_epsilon = 1e-05


def shifted(block, axis, distance):
    devices = range(lax.axis_size(axis))
    route = [(i - distance, i) for i in devices if i - distance in devices]
    return lax.ppermute(block, axis, route)


def expert_backward(x_rows, cot_rows, w_gate, w_up, w_down):
    pre_gate = jnp.dot(x_rows, w_gate, preferred_element_type=jnp.float32)
    pre_up = jnp.dot(x_rows, w_up, preferred_element_type=jnp.float32)
    sig_gate = jax.nn.sigmoid(pre_gate)
    activation = (pre_gate * sig_gate * pre_up).astype(jnp.bfloat16)
    down_g = lax.dot_general(
        activation, cot_rows, (((0,), (0,)), ((), ())), preferred_element_type=jnp.float32
    ).astype(jnp.bfloat16)
    act_grad = lax.dot_general(
        cot_rows, w_down, (((1,), (1,)), ((), ())), preferred_element_type=jnp.float32
    )
    gate_pre_grad = (act_grad * pre_up * sig_gate * (1.0 + pre_gate * (1.0 - sig_gate))).astype(
        jnp.bfloat16
    )
    up_pre_grad = (act_grad * pre_gate * sig_gate).astype(jnp.bfloat16)
    gate_g = lax.dot_general(
        x_rows, gate_pre_grad, (((0,), (0,)), ((), ())), preferred_element_type=jnp.float32
    ).astype(jnp.bfloat16)
    up_g = lax.dot_general(
        x_rows, up_pre_grad, (((0,), (0,)), ((), ())), preferred_element_type=jnp.float32
    ).astype(jnp.bfloat16)
    partial_value = lax.dot_general(
        gate_pre_grad, w_gate, (((1,), (1,)), ((), ())), preferred_element_type=jnp.float32
    )
    partial_value = partial_value + lax.dot_general(
        up_pre_grad, w_up, (((1,), (1,)), ((), ())), preferred_element_type=jnp.float32
    )
    rounded = lax.optimization_barrier(partial_value.astype(jnp.bfloat16))
    return (gate_g, up_g, down_g, rounded.astype(jnp.float32))


def on_device(
    mixer_out,
    conv_out,
    out_cot,
    routes,
    route_weight,
    gate_weight,
    up_weight,
    down_weight,
    out_weight,
    norm_gain,
    conv_taps,
):
    tokens_here, model_width = out_cot.shape
    route_count = routes.shape[1]
    experts = lax.axis_size("sp")
    capacity = 2 * tokens_here * route_count // experts
    quarter = conv_out.shape[1]
    first_col = lax.axis_index("tp") * quarter
    flat_routes = routes.reshape(-1)
    one_hot = (flat_routes[:, None] == jnp.arange(experts, dtype=jnp.int32)[None, :]).astype(
        jnp.int32
    )
    within = jnp.sum((jnp.cumsum(one_hot, axis=0) - one_hot) * one_hot, axis=1)
    slot_index = flat_routes * capacity + within
    row_cot = (route_weight[:, :, None] * out_cot[:, None, :].astype(jnp.float32)).astype(
        jnp.bfloat16
    )
    row_cot = row_cot.reshape(tokens_here * route_count, model_width)
    rows_input = jnp.repeat(mixer_out, route_count, axis=0)
    w_gate = gate_weight[0]
    w_up = up_weight[0]
    w_down = down_weight[0]
    rows_part = lax.dynamic_slice_in_dim(rows_input, first_col, quarter, 1)
    cot_part = lax.dynamic_slice_in_dim(row_cot, first_col, quarter, 1)
    send_rows = jnp.zeros((experts * capacity, quarter), jnp.bfloat16).at[slot_index].set(rows_part)
    send_cot = jnp.zeros((experts * capacity, quarter), jnp.bfloat16).at[slot_index].set(cot_part)
    rows_slice, cot_slice = (
        lax.all_to_all(send_rows, "sp", split_axis=0, concat_axis=0, tiled=True),
        lax.all_to_all(send_cot, "sp", split_axis=0, concat_axis=0, tiled=True),
    )
    x_rows, cot_rows = (
        lax.all_gather(rows_slice, "tp", axis=1, tiled=True),
        lax.all_gather(cot_slice, "tp", axis=1, tiled=True),
    )
    gate_g, up_g, down_g, partial_value = expert_backward(x_rows, cot_rows, w_gate, w_up, w_down)
    back_slice = lax.psum_scatter(
        partial_value.astype(jnp.bfloat16), "tp", scatter_dimension=1, tiled=True
    )
    returned = lax.all_to_all(back_slice, "sp", split_axis=0, concat_axis=0, tiled=True)
    picked = returned[slot_index].astype(jnp.float32).reshape(tokens_here, route_count, quarter)
    own_cot = lax.dynamic_slice_in_dim(out_cot, first_col, quarter, 1).astype(jnp.float32)
    mix_part = (own_cot + jnp.sum(picked, axis=1)).astype(jnp.bfloat16)
    mix_grad = lax.all_gather(mix_part, "tp", axis=1, tiled=True)
    conv_vals = conv_out.astype(jnp.float32)
    power_sum = lax.psum(jnp.sum(conv_vals * conv_vals, axis=1), "tp")
    inv_rms = lax.rsqrt(power_sum / model_width + norm_epsilon)[:, None]
    normed = conv_vals * inv_rms * norm_gain[None, :]
    sig_norm = jax.nn.sigmoid(normed)
    activated = (normed * sig_norm).astype(jnp.bfloat16)
    proj_grad = lax.psum_scatter(
        lax.dot_general(
            mix_grad, activated, (((0,), (0,)), ((), ())), preferred_element_type=jnp.float32
        ),
        "sp",
        scatter_dimension=0,
        tiled=True,
    )
    norm_in_grad = lax.dot_general(
        mix_grad, out_weight, (((1,), (1,)), ((), ())), preferred_element_type=jnp.float32
    )
    scaled = norm_in_grad * sig_norm * (1.0 + normed * (1.0 - sig_norm)) * norm_gain[None, :]
    dot_sum = lax.psum(jnp.sum(conv_vals * scaled, axis=1), "tp")
    conv_grad = inv_rms * scaled - conv_vals * inv_rms**3 * (dot_sum / model_width)[:, None]
    reach = conv_taps.shape[0] - 1
    following = shifted(conv_grad[:reach].astype(jnp.bfloat16), "sp", -1).astype(jnp.float32)
    extended = jnp.concatenate([conv_grad, following], axis=0)
    gated_grad = jnp.zeros((tokens_here, quarter), jnp.float32)
    for tap_index in range(reach + 1):
        gated_grad = (
            gated_grad
            + conv_taps[tap_index][None, :] * extended[tap_index : tap_index + tokens_here]
        )
    return (gate_g[None], up_g[None], down_g[None], proj_grad, gated_grad)


VMEM = pl.BlockSpec(memory_space=pltpu.VMEM)
DMA = pltpu.SemaphoreType.DMA
MESH = pl.DeviceIdType.MESH


def greet(peers):
    barrier = pltpu.get_barrier_semaphore()
    for peer in peers:
        pl.semaphore_signal(barrier, inc=1, device_id=peer, device_id_type=MESH)
    pl.semaphore_wait(barrier, len(peers))


def send(src, dst, send_sem, recv_sem, device):
    return pltpu.make_async_remote_copy(
        src_ref=src,
        dst_ref=dst,
        send_sem=send_sem,
        recv_sem=recv_sem,
        device_id=device,
        device_id_type=MESH,
    )


def places():
    me, q = lax.axis_index("sp"), lax.axis_index("tp")
    twin = q + 1 - 2 * (q % 2)
    across = (q + 2) % 4
    return me, q, twin, across


def params(number):
    return pltpu.CompilerParams(collective_id=number, has_side_effects=True)


def span(index, size):
    return pl.ds(pl.multiple_of(index * size, size), size)


def toggled(value, bits):
    power = 1
    while power <= bits:
        if bits & power:
            value = value + power - 2 * power * ((value // power) % 2)
        power *= 2
    return value


def as_row(column):
    size = column.shape[0]
    same = lax.broadcasted_iota(jnp.int32, (size, size), 0) == lax.broadcasted_iota(jnp.int32, (size, size), 1)
    return jnp.sum(jnp.where(same, column, 0.0), axis=0, keepdims=True)


def as_column(row):
    size = row.shape[1]
    same = lax.broadcasted_iota(jnp.int32, (size, size), 0) == lax.broadcasted_iota(jnp.int32, (size, size), 1)
    return jnp.sum(jnp.where(same, row, 0.0), axis=1, keepdims=True)


def dispatch_kernel(n, x_hbm, cot_hbm, routes_ref, weight_ref, conv_ref, xc_ref, sel_ref, sqs_ref,
                    xq, cq, s_buf, codes, wts, in_sem, own_sem, a_s, a_r, t_s, t_r, x_s, x_r, f_s, f_r, q_s, q_r):
    me, q, twin, across = places()
    twin_across = (twin + 2) % 4
    bf16, f32 = jnp.bfloat16, jnp.float32
    tokens, cols = xq.shape
    rows = s_buf.shape[2]
    loads = [
        pltpu.make_async_copy(x_hbm.at[:, span(q, cols)], xq, in_sem.at[0]),
        pltpu.make_async_copy(cot_hbm.at[:, span(q, cols)], cq, in_sem.at[1]),
    ]
    for c in loads:
        c.start()
    barrier = pltpu.get_barrier_semaphore()
    peers = [(toggled(me, j), q) for j in range(1, n)] + [(me, twin), (me, across), (me, twin_across)]
    for peer in peers:
        pl.semaphore_signal(barrier, inc=1, device_id=peer, device_id_type=MESH)
    height = codes.shape[0]
    which = lax.broadcasted_iota(jnp.int32, (height, tokens), 0)
    member = jnp.zeros((height, tokens), f32)
    weight_of = jnp.zeros((height, tokens), f32)
    for k in range(routes_ref.shape[0]):
        named = routes_ref[pl.ds(k, 1), :] == which
        member = jnp.where(named, 1.0, member)
        weight_of = jnp.where(named, weight_ref[pl.ds(k, 1), :], weight_of)
    earlier = lax.broadcasted_iota(jnp.int32, (tokens, tokens), 0) < lax.broadcasted_iota(
        jnp.int32, (tokens, tokens), 1
    )
    rank = jnp.dot(member.astype(bf16), jnp.where(earlier, 1.0, 0.0).astype(bf16), preferred_element_type=f32)
    codes[...] = jnp.where(member > 0.5, rank, -1.0)
    wts[...] = weight_of
    conv = conv_ref[...].astype(f32)
    squares = as_row(jnp.sum(conv * conv, axis=1, keepdims=True))
    sqs_ref[q] = jnp.broadcast_to(squares, sqs_ref.shape[1:])
    place = lax.broadcasted_iota(jnp.int32, (rows, tokens), 0).astype(f32)
    for c in loads:
        c.wait()
    pending = []
    for j in range(n):
        d = toggled(me, j)
        chosen = codes[pl.ds(d, 1), :] == place
        select = jnp.where(chosen, 1.0, 0.0).astype(bf16)
        scale = jnp.sum(jnp.where(chosen, wts[pl.ds(d, 1), :], 0.0), axis=1, keepdims=True)
        sel_ref[span(d, rows), :] = select
        s_buf[j, 0] = jnp.dot(select, xq[...], preferred_element_type=f32).astype(bf16)
        s_buf[j, 1] = (jnp.dot(select, cq[...], preferred_element_type=f32) * scale).astype(bf16)
        if j == 0:
            pl.semaphore_wait(barrier, len(peers))
            target = xc_ref.at[:, span(me, rows), span(q, cols)]
            own = pltpu.make_async_copy(s_buf.at[0], target, own_sem)
            own.start()
            for part, (sem_s, sem_r, peer) in enumerate(((x_s, x_r, across), (t_s, t_r, twin))):
                c = send(s_buf.at[0], target, sem_s.at[0], sem_r.at[0], (me, peer))
                c.start()
                pending.append(c)
        else:
            c = send(s_buf.at[j], xc_ref.at[:, span(me, rows), span(q, cols)], a_s.at[j], a_r.at[j], (d, q))
            c.start()
            pending.append(c)
    last = [pending[1]]
    small = []
    for k, peer in enumerate((twin, across, twin_across)):
        c = send(sqs_ref.at[q], sqs_ref.at[q], q_s.at[k], q_r.at[k], (me, peer))
        c.start()
        small.append(c)

    def block(j, quarter):
        return xc_ref.at[:, span(toggled(me, j), rows), span(quarter, cols)]

    def relay(j):
        c = send(block(j, across), block(j, across), f_s.at[j], f_r.at[j], (me, twin))
        send(block(j, across), block(j, across), x_s.at[j], x_r.at[j], (me, across)).wait_recv()
        c.start()
        last.append(c)
        pending.append(c)

    for j in range(1, n):
        send(s_buf.at[j], block(j, q), a_s.at[j], a_r.at[j], (me, q)).wait_recv()
        c = send(block(j, q), block(j, q), x_s.at[j], x_r.at[j], (me, across))
        c.start()
        pending.append(c)
        c = send(block(j, q), block(j, q), t_s.at[j], t_r.at[j], (me, twin))
        c.start()
        pending.append(c)
        last.append(c)
        relay(j - 1)
    relay(n - 1)
    own.wait()
    for c in last:
        c.wait_recv()
    for c in small:
        c.wait()
    for c in pending:
        c.wait_send()


def rest_kernel(n, p_ref, sqs_ref, conv_ref, gain_ref, sel_ref, cot_hbm, w_ref, taps_ref, gated_ref, proj_ref,
                act, all_ref, cq, d_r, sx, rx, back, ret, mg, pr, ext, halo, dots, in_sem, d1_s, d1_r, x_s, x_r,
                a_s, a_r, o_sem, up_s, up_r, dn_s, dn_r, y_s, y_r, m_s, m_r, b_s, b_r, e_s, e_r, t_s, t_r, h_s, h_r):
    me, q, twin, across = places()
    twin_across = (twin + 2) % 4
    bf16, f32 = jnp.bfloat16, jnp.float32
    tokens, cols = conv_ref.shape
    rows = ret.shape[0] // n
    level, side = me // 2, me % 2
    mate = me + 1 - 2 * side
    levels = n // 2
    below, above = (me + n - 2) % n, (me + 2) % n
    before = (me + n - 1) % n
    load = pltpu.make_async_copy(cot_hbm.at[:, span(q, cols)], cq, in_sem)
    load.start()
    greet([((me + j) % n, q) for j in range(1, n)] + [(me, twin), (me, across), (me, twin_across)])
    order = list(range(n - 1, -1, -1))
    waits = []
    firsts = {}
    for j in order:
        for k, quarter in enumerate((twin_across, twin)):
            part = span(toggled(me, j), rows)
            c = send(p_ref.at[part, span(quarter, cols)], d_r.at[k, part], d1_s.at[k, j], d1_r.at[k, j], (me, twin))
            c.start()
            firsts[k, j] = c
            waits.append(c)
    conv = conv_ref[...].astype(f32)
    gain = gain_ref[...]
    power = as_column((sqs_ref[0] + sqs_ref[1] + sqs_ref[2] + sqs_ref[3])[:1])
    inv = lax.rsqrt(power / (cols * 4) + norm_epsilon)
    normed = conv * inv * gain
    act[...] = (normed * jax.nn.sigmoid(normed)).astype(bf16)

    def piece(lvl):
        return all_ref.at[span((lvl + levels) % levels * 2 + side, tokens)]

    def ways(t):
        up = send(act if t == 0 else piece(level - t), piece(level - t), up_s.at[t], up_r.at[t], (above, q))
        dn = send(act if t == 0 else piece(level + t), piece(level + t), dn_s.at[t], dn_r.at[t], (below, q))
        return up, dn

    def over(k, lvl):
        src = act if k == 0 else piece(lvl)
        return send(src, piece(lvl), y_s.at[k], y_r.at[k], (mate, q))

    def start_ways(t):
        up, dn = ways(t)
        pl.when(jnp.logical_and(level - t >= 0, level + 1 < levels))(up.start)
        pl.when(jnp.logical_and(level + t < levels, level >= 1))(dn.start)

    def take(t):
        got_up = send(act, piece(level - 1 - t), up_s.at[t], up_r.at[t], (above, q))
        got_dn = send(act, piece(level + 1 + t), dn_s.at[t], dn_r.at[t], (below, q))

        @pl.when(level - 1 - t >= 0)
        def _():
            got_up.wait_recv()
            over(1 + t, level - 1 - t).start()

        @pl.when(level + 1 + t < levels)
        def _():
            got_dn.wait_recv()
            over(levels + t, level + 1 + t).start()

    def first(j):
        part = span(toggled(me, j), rows)
        firsts[0, j].wait_recv()
        near = p_ref[part, span(across, cols)].astype(f32) + d_r[0, part].astype(f32)
        sx[part] = near.astype(bf16)
        c = send(sx.at[part], rx.at[part], x_s.at[j], x_r.at[j], (me, across))
        c.start()
        waits.append(c)
        return c

    def second(j, c):
        part = span(toggled(me, j), rows)
        firsts[1, j].wait_recv()
        total = p_ref[part, span(q, cols)].astype(f32) + d_r[1, part].astype(f32)
        c.wait_recv()
        total = (total + rx[part].astype(f32)).astype(bf16)
        if j == 0:
            ret[part] = total
        else:
            back[part] = total
            out = send(back.at[part], ret.at[span(me, rows)], a_s.at[j], a_r.at[j], (toggled(me, j), q))
            out.start()
            waits.append(out)

    crossing = [first(j) for j in order[:2]]
    start_ways(0)
    over(0, level).start()
    own = pltpu.make_async_copy(act, all_ref.at[span(me, tokens)], o_sem.at[0])
    own.start()
    crossing += [first(j) for j in order[2:]]
    for at, j in enumerate(order):
        second(j, crossing[at])
        if at == 1:
            take(0)
            start_ways(1)
        if at == 4:
            take(1)
            start_ways(2)
    load.wait()
    for j in order[:-1]:
        got = send(back.at[span(me, rows)], ret.at[span(toggled(me, j), rows)], a_s.at[j], a_r.at[j], (me, q))
        got.wait_recv()

    summed = lax.dot_general(sel_ref[...], ret[...], (((0,), (0,)), ((), ())), preferred_element_type=f32)
    mg[:, span(q, cols)] = (cq[...].astype(f32) + summed).astype(bf16)
    mine = mg.at[:, span(q, cols)]
    to_x = send(mine, mine, m_s.at[0], m_r.at[0], (me, across))
    to_x.start()
    to_twin = send(mine, mine, m_s.at[1], m_r.at[1], (me, twin))
    to_twin.start()
    take(2)
    sig = jax.nn.sigmoid(normed)
    slope = sig * (1.0 + normed * (1.0 - sig)) * gain
    theirs = mg.at[:, span(across, cols)]
    to_x.wait_recv()
    relay = send(theirs, theirs, m_s.at[2], m_r.at[2], (me, twin))
    relay.start()
    to_twin.wait_recv()
    relay.wait_recv()
    waits += [to_x, to_twin, relay]
    share, block = pr.shape[2], pr.shape[3]
    incoming = []
    for j in order[:-1]:
        d = toggled(me, j)
        c = send(mg.at[span(q, share), span(d, block)], pr.at[me, q], b_s.at[j], b_r.at[j], (d, q))
        c.start()
        waits.append(c)
        incoming.append(send(mg.at[span(q, share), span(d, block)], pr.at[d, q], b_s.at[j], b_r.at[j], (d, q)))
    kept = pltpu.make_async_copy(mg.at[span(q, share), span(me, block)], pr.at[me, q], o_sem.at[1])
    kept.start()
    into = lax.dot_general(mg[...], w_ref[...], (((1,), (1,)), ((), ())), preferred_element_type=f32)
    scaled = into * slope
    dots[0] = jnp.broadcast_to(as_row(jnp.sum(conv * scaled, axis=1, keepdims=True)), dots.shape[1:])
    small = []
    for k, peer in enumerate((twin, across, twin_across)):
        c = send(dots.at[0], dots.at[k + 1], t_s.at[k], t_r.at[k], (me, peer))
        c.start()
        small.append(c)
    ext[pl.ds(0, tokens)] = inv * scaled
    kept.wait()
    for c in incoming:
        c.wait_recv()
    spread = [
        send(pr.at[:, q], pr.at[:, q], e_s.at[0], e_r.at[0], (me, across)),
        send(pr.at[:, q], pr.at[:, q], e_s.at[1], e_r.at[1], (me, twin)),
        send(pr.at[:, across], pr.at[:, across], e_s.at[2], e_r.at[2], (me, twin)),
    ]
    spread[0].start()
    spread[1].start()
    for c in small:
        c.wait()
    total = as_column((dots[0] + dots[1] + dots[2] + dots[3])[:1])
    grad = ext[pl.ds(0, tokens)] - conv * (inv * inv * inv * (total / (cols * 4)))
    ext[pl.ds(0, tokens)] = grad
    pad = halo.shape[1]
    halo[0] = grad[:pad].astype(bf16)
    shift = send(halo.at[0], halo.at[1], h_s, h_r, (before, q))
    pl.when(me > 0)(shift.start)
    spread[0].wait_recv()
    spread[2].start()

    @pl.when(me < n - 1)
    def _():
        shift.wait_recv()
        ext[pl.ds(tokens, pad)] = halo[1].astype(f32)

    @pl.when(me == n - 1)
    def _():
        ext[pl.ds(tokens, pad)] = jnp.zeros((pad, cols), f32)

    step = 128
    for low in range(0, cols, step):
        band = pl.ds(low, step)
        acc = taps_ref[pl.ds(0, 1), band] * ext[pl.ds(0, tokens), band]
        for tap in range(1, taps_ref.shape[0]):
            acc = acc + taps_ref[pl.ds(tap, 1), band] * ext[pl.ds(tap, tokens), band]
        gated_ref[:, band] = acc

    def other(lvl):
        return all_ref.at[span((lvl + levels) % levels * 2 + 1 - side, tokens)]

    for t in range(levels - 1):
        up, dn = ways(t)
        pl.when(jnp.logical_and(level - t >= 0, level + 1 < levels))(up.wait_send)
        pl.when(jnp.logical_and(level + t < levels, level >= 1))(dn.wait_send)
    for k in range(2 * levels - 1):
        lvl = level - k if k < levels else level + k - levels + 1
        here = lvl >= 0 if k < levels else lvl < levels

        @pl.when(here)
        def _():
            over(k, lvl).wait_send()
            send(act, other(lvl), y_s.at[k], y_r.at[k], (mate, q)).wait_recv()

    own.wait()
    spread[1].wait_recv()
    spread[2].wait_recv()
    proj_ref[...] = lax.dot_general(
        pr[...].reshape(n * tokens, block), all_ref[...], (((0,), (0,)), ((), ())), preferred_element_type=f32
    )
    pl.when(me > 0)(shift.wait_send)
    for c in spread:
        c.wait_send()
    for c in waits:
        c.wait_send()


def near_plan(mixer_out, conv_out, out_cot, routes, route_weight, gate_weight, up_weight, down_weight, out_weight,
              norm_gain, conv_taps):
    tokens_here, model_width = out_cot.shape
    n = lax.axis_size("sp")
    capacity = 2 * tokens_here * routes.shape[1] // n
    quarter = conv_out.shape[1]
    bf16, f32 = jnp.bfloat16, jnp.float32
    total_rows = n * capacity
    shape = jax.ShapeDtypeStruct
    anywhere = pl.BlockSpec(memory_space=pl.ANY)
    height = -(-n // 16) * 16
    x_and_cot, select, squares = pl.pallas_call(
        functools.partial(dispatch_kernel, n),
        out_shape=(
            shape((2, total_rows, model_width), bf16),
            shape((total_rows, tokens_here), bf16),
            shape((4, 8, tokens_here), f32),
        ),
        in_specs=[anywhere] * 2 + [VMEM] * 3,
        out_specs=(VMEM, VMEM, VMEM),
        scratch_shapes=[pltpu.VMEM((tokens_here, quarter), bf16)] * 2
        + [pltpu.VMEM((n, 2, capacity, quarter), bf16)]
        + [pltpu.VMEM((height, tokens_here), f32)] * 2
        + [DMA((2,)), DMA]
        + [DMA((n,))] * 8
        + [DMA((3,))] * 2,
        compiler_params=params(0),
        name="dispatch",
    )(mixer_out, out_cot, routes.T, route_weight.T, conv_out)
    gate_g, up_g, down_g, partial_value = expert_backward(
        x_and_cot[0], x_and_cot[1], gate_weight[0], up_weight[0], down_weight[0]
    )
    levels = n // 2
    pad = -(-(conv_taps.shape[0] - 1) // 16) * 16
    gated_grad, proj_grad = pl.pallas_call(
        functools.partial(rest_kernel, n),
        out_shape=(shape((tokens_here, quarter), f32), shape((model_width // n, quarter), f32)),
        in_specs=[VMEM] * 5 + [anywhere] + [VMEM] * 2,
        out_specs=(VMEM, VMEM),
        scratch_shapes=[
            pltpu.VMEM((tokens_here, quarter), bf16),
            pltpu.VMEM((n * tokens_here, quarter), bf16),
            pltpu.VMEM((tokens_here, quarter), bf16),
            pltpu.VMEM((2, total_rows, quarter), bf16),
        ]
        + [pltpu.VMEM((total_rows, quarter), bf16)] * 4
        + [
            pltpu.VMEM((tokens_here, model_width), bf16),
            pltpu.VMEM((n, 4, tokens_here // 4, model_width // n), bf16),
            pltpu.VMEM((tokens_here + pad, quarter), f32),
            pltpu.VMEM((2, pad, quarter), bf16),
            pltpu.VMEM((4, 8, tokens_here), f32),
            DMA,
        ]
        + [DMA((2, n))] * 2
        + [DMA((n,))] * 4
        + [DMA((2,))]
        + [DMA((levels,))] * 4
        + [DMA((2 * levels,))] * 2
        + [DMA((3,))] * 2
        + [DMA((n,))] * 2
        + [DMA((3,))] * 4
        + [DMA] * 2,
        compiler_params=params(1),
        name="rest",
    )(partial_value.astype(bf16), squares, conv_out, norm_gain[None, :], select, out_cot, out_weight, conv_taps)
    return (gate_g[None], up_g[None], down_g[None], proj_grad, gated_grad)


def either_plan(*arrays):
    near = lax.axis_size("tp") == 4 and lax.axis_size("sp") == 8
    return near_plan(*arrays) if near else on_device(*arrays)


def solution(mesh):
    placed = (
        P("sp", None),
        P("sp", "tp"),
        P("sp", None),
        P("sp", None),
        P("sp", None),
        P("sp", None, "tp"),
        P("sp", None, "tp"),
        P("sp", "tp", None),
        P("tp", None),
        P("tp"),
        P(None, "tp"),
    )
    return jax.shard_map(
        either_plan,
        mesh=mesh,
        in_specs=placed,
        out_specs=(
            P("sp", None, "tp"),
            P("sp", None, "tp"),
            P("sp", "tp", None),
            P("sp", "tp"),
            P("sp", "tp"),
        ),
        check_vma=False,
    )
```

```python
import functools

import jax
import jax.numpy as jnp
from jax import lax
from jax.experimental import pallas as pl
from jax.experimental.pallas import tpu as pltpu
from jax.sharding import PartitionSpec as P

norm_epsilon = 1e-05


def shifted(block, axis, distance):
    devices = range(lax.axis_size(axis))
    route = [(i - distance, i) for i in devices if i - distance in devices]
    return lax.ppermute(block, axis, route)


def expert_backward(x_rows, cot_rows, w_gate, w_up, w_down):
    pre_gate = jnp.dot(x_rows, w_gate, preferred_element_type=jnp.float32)
    pre_up = jnp.dot(x_rows, w_up, preferred_element_type=jnp.float32)
    sig_gate = jax.nn.sigmoid(pre_gate)
    activation = (pre_gate * sig_gate * pre_up).astype(jnp.bfloat16)
    down_g = lax.dot_general(
        activation, cot_rows, (((0,), (0,)), ((), ())), preferred_element_type=jnp.float32
    ).astype(jnp.bfloat16)
    act_grad = lax.dot_general(
        cot_rows, w_down, (((1,), (1,)), ((), ())), preferred_element_type=jnp.float32
    )
    gate_pre_grad = (act_grad * pre_up * sig_gate * (1.0 + pre_gate * (1.0 - sig_gate))).astype(
        jnp.bfloat16
    )
    up_pre_grad = (act_grad * pre_gate * sig_gate).astype(jnp.bfloat16)
    gate_g = lax.dot_general(
        x_rows, gate_pre_grad, (((0,), (0,)), ((), ())), preferred_element_type=jnp.float32
    ).astype(jnp.bfloat16)
    up_g = lax.dot_general(
        x_rows, up_pre_grad, (((0,), (0,)), ((), ())), preferred_element_type=jnp.float32
    ).astype(jnp.bfloat16)
    partial_value = lax.dot_general(
        gate_pre_grad, w_gate, (((1,), (1,)), ((), ())), preferred_element_type=jnp.float32
    )
    partial_value = partial_value + lax.dot_general(
        up_pre_grad, w_up, (((1,), (1,)), ((), ())), preferred_element_type=jnp.float32
    )
    rounded = lax.optimization_barrier(partial_value.astype(jnp.bfloat16))
    return (gate_g, up_g, down_g, rounded.astype(jnp.float32))


def on_device(
    mixer_out,
    conv_out,
    out_cot,
    routes,
    route_weight,
    gate_weight,
    up_weight,
    down_weight,
    out_weight,
    norm_gain,
    conv_taps,
):
    tokens_here, model_width = out_cot.shape
    route_count = routes.shape[1]
    experts = lax.axis_size("sp")
    capacity = 2 * tokens_here * route_count // experts
    quarter = conv_out.shape[1]
    first_col = lax.axis_index("tp") * quarter
    flat_routes = routes.reshape(-1)
    one_hot = (flat_routes[:, None] == jnp.arange(experts, dtype=jnp.int32)[None, :]).astype(
        jnp.int32
    )
    within = jnp.sum((jnp.cumsum(one_hot, axis=0) - one_hot) * one_hot, axis=1)
    slot_index = flat_routes * capacity + within
    row_cot = (route_weight[:, :, None] * out_cot[:, None, :].astype(jnp.float32)).astype(
        jnp.bfloat16
    )
    row_cot = row_cot.reshape(tokens_here * route_count, model_width)
    rows_input = jnp.repeat(mixer_out, route_count, axis=0)
    w_gate = gate_weight[0]
    w_up = up_weight[0]
    w_down = down_weight[0]
    rows_part = lax.dynamic_slice_in_dim(rows_input, first_col, quarter, 1)
    cot_part = lax.dynamic_slice_in_dim(row_cot, first_col, quarter, 1)
    send_rows = jnp.zeros((experts * capacity, quarter), jnp.bfloat16).at[slot_index].set(rows_part)
    send_cot = jnp.zeros((experts * capacity, quarter), jnp.bfloat16).at[slot_index].set(cot_part)
    rows_slice, cot_slice = (
        lax.all_to_all(send_rows, "sp", split_axis=0, concat_axis=0, tiled=True),
        lax.all_to_all(send_cot, "sp", split_axis=0, concat_axis=0, tiled=True),
    )
    x_rows, cot_rows = (
        lax.all_gather(rows_slice, "tp", axis=1, tiled=True),
        lax.all_gather(cot_slice, "tp", axis=1, tiled=True),
    )
    gate_g, up_g, down_g, partial_value = expert_backward(x_rows, cot_rows, w_gate, w_up, w_down)
    back_slice = lax.psum_scatter(
        partial_value.astype(jnp.bfloat16), "tp", scatter_dimension=1, tiled=True
    )
    returned = lax.all_to_all(back_slice, "sp", split_axis=0, concat_axis=0, tiled=True)
    picked = returned[slot_index].astype(jnp.float32).reshape(tokens_here, route_count, quarter)
    own_cot = lax.dynamic_slice_in_dim(out_cot, first_col, quarter, 1).astype(jnp.float32)
    mix_part = (own_cot + jnp.sum(picked, axis=1)).astype(jnp.bfloat16)
    mix_grad = lax.all_gather(mix_part, "tp", axis=1, tiled=True)
    conv_vals = conv_out.astype(jnp.float32)
    power_sum = lax.psum(jnp.sum(conv_vals * conv_vals, axis=1), "tp")
    inv_rms = lax.rsqrt(power_sum / model_width + norm_epsilon)[:, None]
    normed = conv_vals * inv_rms * norm_gain[None, :]
    sig_norm = jax.nn.sigmoid(normed)
    activated = (normed * sig_norm).astype(jnp.bfloat16)
    proj_grad = lax.psum_scatter(
        lax.dot_general(
            mix_grad, activated, (((0,), (0,)), ((), ())), preferred_element_type=jnp.float32
        ),
        "sp",
        scatter_dimension=0,
        tiled=True,
    )
    norm_in_grad = lax.dot_general(
        mix_grad, out_weight, (((1,), (1,)), ((), ())), preferred_element_type=jnp.float32
    )
    scaled = norm_in_grad * sig_norm * (1.0 + normed * (1.0 - sig_norm)) * norm_gain[None, :]
    dot_sum = lax.psum(jnp.sum(conv_vals * scaled, axis=1), "tp")
    conv_grad = inv_rms * scaled - conv_vals * inv_rms**3 * (dot_sum / model_width)[:, None]
    reach = conv_taps.shape[0] - 1
    following = shifted(conv_grad[:reach].astype(jnp.bfloat16), "sp", -1).astype(jnp.float32)
    extended = jnp.concatenate([conv_grad, following], axis=0)
    gated_grad = jnp.zeros((tokens_here, quarter), jnp.float32)
    for tap_index in range(reach + 1):
        gated_grad = (
            gated_grad
            + conv_taps[tap_index][None, :] * extended[tap_index : tap_index + tokens_here]
        )
    return (gate_g[None], up_g[None], down_g[None], proj_grad, gated_grad)


VMEM = pl.BlockSpec(memory_space=pltpu.VMEM)
DMA = pltpu.SemaphoreType.DMA
MESH = pl.DeviceIdType.MESH


def greet(peers):
    barrier = pltpu.get_barrier_semaphore()
    for peer in peers:
        pl.semaphore_signal(barrier, inc=1, device_id=peer, device_id_type=MESH)
    pl.semaphore_wait(barrier, len(peers))


def send(src, dst, send_sem, recv_sem, device):
    return pltpu.make_async_remote_copy(
        src_ref=src,
        dst_ref=dst,
        send_sem=send_sem,
        recv_sem=recv_sem,
        device_id=device,
        device_id_type=MESH,
    )


def places():
    me, q = lax.axis_index("sp"), lax.axis_index("tp")
    twin = q + 1 - 2 * (q % 2)
    across = (q + 2) % 4
    return me, q, twin, across


def params(number):
    return pltpu.CompilerParams(collective_id=number, has_side_effects=True)


def span(index, size):
    return pl.ds(pl.multiple_of(index * size, size), size)


def toggled(value, bits):
    power = 1
    while power <= bits:
        if bits & power:
            value = value + power - 2 * power * ((value // power) % 2)
        power *= 2
    return value


def as_row(column):
    size = column.shape[0]
    same = lax.broadcasted_iota(jnp.int32, (size, size), 0) == lax.broadcasted_iota(jnp.int32, (size, size), 1)
    return jnp.sum(jnp.where(same, column, 0.0), axis=0, keepdims=True)


def as_column(row):
    size = row.shape[1]
    same = lax.broadcasted_iota(jnp.int32, (size, size), 0) == lax.broadcasted_iota(jnp.int32, (size, size), 1)
    return jnp.sum(jnp.where(same, row, 0.0), axis=1, keepdims=True)


def dispatch_kernel(n, x_hbm, cot_hbm, routes_ref, weight_ref, conv_ref, xc_ref, sel_ref, sqs_ref,
                    xq, cq, s_buf, codes, wts, in_sem, own_sem, a_s, a_r, t_s, t_r, x_s, x_r, f_s, f_r, q_s, q_r):
    me, q, twin, across = places()
    twin_across = (twin + 2) % 4
    bf16, f32 = jnp.bfloat16, jnp.float32
    tokens, cols = xq.shape
    rows = s_buf.shape[2]
    loads = [
        pltpu.make_async_copy(x_hbm.at[:, span(q, cols)], xq, in_sem.at[0]),
        pltpu.make_async_copy(cot_hbm.at[:, span(q, cols)], cq, in_sem.at[1]),
    ]
    for c in loads:
        c.start()
    barrier = pltpu.get_barrier_semaphore()
    peers = [(toggled(me, j), q) for j in range(1, n)] + [(me, twin), (me, across), (me, twin_across)]
    for peer in peers:
        pl.semaphore_signal(barrier, inc=1, device_id=peer, device_id_type=MESH)
    height = codes.shape[0]
    which = lax.broadcasted_iota(jnp.int32, (height, tokens), 0)
    member = jnp.zeros((height, tokens), f32)
    weight_of = jnp.zeros((height, tokens), f32)
    for k in range(routes_ref.shape[0]):
        named = routes_ref[pl.ds(k, 1), :] == which
        member = jnp.where(named, 1.0, member)
        weight_of = jnp.where(named, weight_ref[pl.ds(k, 1), :], weight_of)
    earlier = lax.broadcasted_iota(jnp.int32, (tokens, tokens), 0) < lax.broadcasted_iota(
        jnp.int32, (tokens, tokens), 1
    )
    rank = jnp.dot(member.astype(bf16), jnp.where(earlier, 1.0, 0.0).astype(bf16), preferred_element_type=f32)
    codes[...] = jnp.where(member > 0.5, rank, -1.0)
    wts[...] = weight_of
    conv = conv_ref[...].astype(f32)
    squares = as_row(jnp.sum(conv * conv, axis=1, keepdims=True))
    sqs_ref[q] = jnp.broadcast_to(squares, sqs_ref.shape[1:])
    place = lax.broadcasted_iota(jnp.int32, (rows, tokens), 0).astype(f32)
    for c in loads:
        c.wait()
    pending = []
    for j in range(n):
        d = toggled(me, j)
        chosen = codes[pl.ds(d, 1), :] == place
        select = jnp.where(chosen, 1.0, 0.0).astype(bf16)
        scale = jnp.sum(jnp.where(chosen, wts[pl.ds(d, 1), :], 0.0), axis=1, keepdims=True)
        sel_ref[span(d, rows), :] = select
        s_buf[j, 0] = jnp.dot(select, xq[...], preferred_element_type=f32).astype(bf16)
        s_buf[j, 1] = (jnp.dot(select, cq[...], preferred_element_type=f32) * scale).astype(bf16)
        if j == 0:
            pl.semaphore_wait(barrier, len(peers))
            target = xc_ref.at[:, span(me, rows), span(q, cols)]
            own = pltpu.make_async_copy(s_buf.at[0], target, own_sem)
            own.start()
            for part, (sem_s, sem_r, peer) in enumerate(((x_s, x_r, across), (t_s, t_r, twin))):
                c = send(s_buf.at[0], target, sem_s.at[0], sem_r.at[0], (me, peer))
                c.start()
                pending.append(c)
        else:
            c = send(s_buf.at[j], xc_ref.at[:, span(me, rows), span(q, cols)], a_s.at[j], a_r.at[j], (d, q))
            c.start()
            pending.append(c)
    last = [pending[1]]
    small = []
    for k, peer in enumerate((twin, across, twin_across)):
        c = send(sqs_ref.at[q], sqs_ref.at[q], q_s.at[k], q_r.at[k], (me, peer))
        c.start()
        small.append(c)

    def block(j, quarter):
        return xc_ref.at[:, span(toggled(me, j), rows), span(quarter, cols)]

    def relay(j):
        c = send(block(j, across), block(j, across), f_s.at[j], f_r.at[j], (me, twin))
        send(block(j, across), block(j, across), x_s.at[j], x_r.at[j], (me, across)).wait_recv()
        c.start()
        last.append(c)
        pending.append(c)

    for j in range(1, n):
        send(s_buf.at[j], block(j, q), a_s.at[j], a_r.at[j], (me, q)).wait_recv()
        c = send(block(j, q), block(j, q), x_s.at[j], x_r.at[j], (me, across))
        c.start()
        pending.append(c)
        c = send(block(j, q), block(j, q), t_s.at[j], t_r.at[j], (me, twin))
        c.start()
        pending.append(c)
        last.append(c)
        relay(j - 1)
    relay(n - 1)
    own.wait()
    for c in last:
        c.wait_recv()
    for c in small:
        c.wait()
    for c in pending:
        c.wait_send()


def rest_kernel(n, p_ref, sqs_ref, conv_ref, gain_ref, sel_ref, cot_hbm, w_hbm, taps_ref, gated_ref, proj_ref,
                act, all_ref, cq, w_buf, d_r, sx, rx, back, ret, mg, pr, ext, halo, dots, in_sem, w_sem, d1_s, d1_r, x_s, x_r,
                a_s, a_r, o_sem, up_s, up_r, dn_s, dn_r, y_s, y_r, m_s, m_r, b_s, b_r, e_s, e_r, t_s, t_r, h_s, h_r):
    me, q, twin, across = places()
    twin_across = (twin + 2) % 4
    bf16, f32 = jnp.bfloat16, jnp.float32
    tokens, cols = conv_ref.shape
    rows = ret.shape[0] // n
    level, side = me // 2, me % 2
    mate = me + 1 - 2 * side
    levels = n // 2
    below, above = (me + n - 2) % n, (me + 2) % n
    before = (me + n - 1) % n
    load = pltpu.make_async_copy(cot_hbm.at[:, span(q, cols)], cq, in_sem)
    load.start()
    w_load = pltpu.make_async_copy(w_hbm, w_buf, w_sem)
    w_load.start()
    greet([((me + j) % n, q) for j in range(1, n)] + [(me, twin), (me, across), (me, twin_across)])
    order = list(range(n - 1, -1, -1))
    waits = []
    firsts = {}
    for k, quarter in enumerate((twin_across, twin)):
        for j in order:
            part = span(toggled(me, j), rows)
            c = send(p_ref.at[part, span(quarter, cols)], d_r.at[k, part], d1_s.at[k, j], d1_r.at[k, j], (me, twin))
            c.start()
            firsts[k, j] = c
            waits.append(c)
    conv = conv_ref[...].astype(f32)
    gain = gain_ref[...]
    power = as_column((sqs_ref[0] + sqs_ref[1] + sqs_ref[2] + sqs_ref[3])[:1])
    inv = lax.rsqrt(power / (cols * 4) + norm_epsilon)
    normed = conv * inv * gain
    act[...] = (normed * jax.nn.sigmoid(normed)).astype(bf16)

    def piece(lvl):
        return all_ref.at[span((lvl + levels) % levels * 2 + side, tokens)]

    def ways(t):
        up = send(act if t == 0 else piece(level - t), piece(level - t), up_s.at[t], up_r.at[t], (above, q))
        dn = send(act if t == 0 else piece(level + t), piece(level + t), dn_s.at[t], dn_r.at[t], (below, q))
        return up, dn

    def over(k, lvl):
        src = act if k == 0 else piece(lvl)
        return send(src, piece(lvl), y_s.at[k], y_r.at[k], (mate, q))

    def start_ways(t):
        up, dn = ways(t)
        pl.when(jnp.logical_and(level - t >= 0, level + 1 < levels))(up.start)
        pl.when(jnp.logical_and(level + t < levels, level >= 1))(dn.start)

    def take(t):
        got_up = send(act, piece(level - 1 - t), up_s.at[t], up_r.at[t], (above, q))
        got_dn = send(act, piece(level + 1 + t), dn_s.at[t], dn_r.at[t], (below, q))

        @pl.when(level - 1 - t >= 0)
        def _():
            got_up.wait_recv()
            over(1 + t, level - 1 - t).start()

        @pl.when(level + 1 + t < levels)
        def _():
            got_dn.wait_recv()
            over(levels + t, level + 1 + t).start()

    def first(j):
        part = span(toggled(me, j), rows)
        firsts[0, j].wait_recv()
        near = p_ref[part, span(across, cols)].astype(f32) + d_r[0, part].astype(f32)
        sx[part] = near.astype(bf16)
        c = send(sx.at[part], rx.at[part], x_s.at[j], x_r.at[j], (me, across))
        c.start()
        waits.append(c)
        return c

    def second(j, c):
        part = span(toggled(me, j), rows)
        firsts[1, j].wait_recv()
        total = p_ref[part, span(q, cols)].astype(f32) + d_r[1, part].astype(f32)
        c.wait_recv()
        total = (total + rx[part].astype(f32)).astype(bf16)
        if j == 0:
            ret[part] = total
        else:
            back[part] = total
            out = send(back.at[part], ret.at[span(me, rows)], a_s.at[j], a_r.at[j], (toggled(me, j), q))
            out.start()
            waits.append(out)

    crossing = [first(j) for j in order[:2]]
    start_ways(0)
    over(0, level).start()
    own = pltpu.make_async_copy(act, all_ref.at[span(me, tokens)], o_sem.at[0])
    own.start()
    crossing += [first(j) for j in order[2:]]
    for at, j in enumerate(order):
        second(j, crossing[at])
    take(0)
    start_ways(1)
    load.wait()
    for j in order[:-1]:
        got = send(back.at[span(me, rows)], ret.at[span(toggled(me, j), rows)], a_s.at[j], a_r.at[j], (me, q))
        got.wait_recv()

    summed = lax.dot_general(sel_ref[...], ret[...], (((0,), (0,)), ((), ())), preferred_element_type=f32)
    mg[:, span(q, cols)] = (cq[...].astype(f32) + summed).astype(bf16)
    mine = mg.at[:, span(q, cols)]
    to_x = send(mine, mine, m_s.at[0], m_r.at[0], (me, across))
    to_x.start()
    to_twin = send(mine, mine, m_s.at[1], m_r.at[1], (me, twin))
    to_twin.start()
    take(1)
    sig = jax.nn.sigmoid(normed)
    slope = sig * (1.0 + normed * (1.0 - sig)) * gain
    theirs = mg.at[:, span(across, cols)]
    to_x.wait_recv()
    relay = send(theirs, theirs, m_s.at[2], m_r.at[2], (me, twin))
    relay.start()
    to_twin.wait_recv()
    relay.wait_recv()
    waits += [to_x, to_twin, relay]
    share, block = pr.shape[2], pr.shape[3]
    incoming = []
    for j in order[:-1]:
        d = toggled(me, j)
        c = send(mg.at[span(q, share), span(d, block)], pr.at[me, q], b_s.at[j], b_r.at[j], (d, q))
        c.start()
        waits.append(c)
        incoming.append(send(mg.at[span(q, share), span(d, block)], pr.at[d, q], b_s.at[j], b_r.at[j], (d, q)))
    kept = pltpu.make_async_copy(mg.at[span(q, share), span(me, block)], pr.at[me, q], o_sem.at[1])
    kept.start()
    start_ways(2)
    w_load.wait()
    into = lax.dot_general(mg[...], w_buf[...], (((1,), (1,)), ((), ())), preferred_element_type=f32)
    scaled = into * slope
    dots[0] = jnp.broadcast_to(as_row(jnp.sum(conv * scaled, axis=1, keepdims=True)), dots.shape[1:])
    small = []
    for k, peer in enumerate((twin, across, twin_across)):
        c = send(dots.at[0], dots.at[k + 1], t_s.at[k], t_r.at[k], (me, peer))
        c.start()
        small.append(c)
    ext[pl.ds(0, tokens)] = inv * scaled
    kept.wait()
    for c in incoming:
        c.wait_recv()
    spread = [
        send(pr.at[:, q], pr.at[:, q], e_s.at[0], e_r.at[0], (me, across)),
        send(pr.at[:, q], pr.at[:, q], e_s.at[1], e_r.at[1], (me, twin)),
        send(pr.at[:, across], pr.at[:, across], e_s.at[2], e_r.at[2], (me, twin)),
    ]
    spread[0].start()
    spread[1].start()
    for c in small:
        c.wait()
    total = as_column((dots[0] + dots[1] + dots[2] + dots[3])[:1])
    grad = ext[pl.ds(0, tokens)] - conv * (inv * inv * inv * (total / (cols * 4)))
    ext[pl.ds(0, tokens)] = grad
    pad = halo.shape[1]
    halo[0] = grad[:pad].astype(bf16)
    shift = send(halo.at[0], halo.at[1], h_s, h_r, (before, q))
    pl.when(me > 0)(shift.start)
    spread[0].wait_recv()
    spread[2].start()
    take(2)

    @pl.when(me < n - 1)
    def _():
        shift.wait_recv()
        ext[pl.ds(tokens, pad)] = halo[1].astype(f32)

    @pl.when(me == n - 1)
    def _():
        ext[pl.ds(tokens, pad)] = jnp.zeros((pad, cols), f32)

    step = 128
    for low in range(0, cols, step):
        band = pl.ds(low, step)
        acc = taps_ref[pl.ds(0, 1), band] * ext[pl.ds(0, tokens), band]
        for tap in range(1, taps_ref.shape[0]):
            acc = acc + taps_ref[pl.ds(tap, 1), band] * ext[pl.ds(tap, tokens), band]
        gated_ref[:, band] = acc

    def other(lvl):
        return all_ref.at[span((lvl + levels) % levels * 2 + 1 - side, tokens)]

    for t in range(levels - 1):
        up, dn = ways(t)
        pl.when(jnp.logical_and(level - t >= 0, level + 1 < levels))(up.wait_send)
        pl.when(jnp.logical_and(level + t < levels, level >= 1))(dn.wait_send)
    for k in range(2 * levels - 1):
        lvl = level - k if k < levels else level + k - levels + 1
        here = lvl >= 0 if k < levels else lvl < levels

        @pl.when(here)
        def _():
            over(k, lvl).wait_send()
            send(act, other(lvl), y_s.at[k], y_r.at[k], (mate, q)).wait_recv()

    own.wait()
    spread[1].wait_recv()
    spread[2].wait_recv()
    proj_ref[...] = lax.dot_general(
        pr[...].reshape(n * tokens, block), all_ref[...], (((0,), (0,)), ((), ())), preferred_element_type=f32
    )
    pl.when(me > 0)(shift.wait_send)
    for c in spread:
        c.wait_send()
    for c in waits:
        c.wait_send()


def near_plan(mixer_out, conv_out, out_cot, routes, route_weight, gate_weight, up_weight, down_weight, out_weight,
              norm_gain, conv_taps):
    tokens_here, model_width = out_cot.shape
    n = lax.axis_size("sp")
    capacity = 2 * tokens_here * routes.shape[1] // n
    quarter = conv_out.shape[1]
    bf16, f32 = jnp.bfloat16, jnp.float32
    total_rows = n * capacity
    shape = jax.ShapeDtypeStruct
    anywhere = pl.BlockSpec(memory_space=pl.ANY)
    height = -(-n // 16) * 16
    x_and_cot, select, squares = pl.pallas_call(
        functools.partial(dispatch_kernel, n),
        out_shape=(
            shape((2, total_rows, model_width), bf16),
            shape((total_rows, tokens_here), bf16),
            shape((4, 8, tokens_here), f32),
        ),
        in_specs=[anywhere] * 2 + [VMEM] * 3,
        out_specs=(VMEM, VMEM, VMEM),
        scratch_shapes=[pltpu.VMEM((tokens_here, quarter), bf16)] * 2
        + [pltpu.VMEM((n, 2, capacity, quarter), bf16)]
        + [pltpu.VMEM((height, tokens_here), f32)] * 2
        + [DMA((2,)), DMA]
        + [DMA((n,))] * 8
        + [DMA((3,))] * 2,
        compiler_params=params(0),
        name="dispatch",
    )(mixer_out, out_cot, routes.T, route_weight.T, conv_out)
    gate_g, up_g, down_g, partial_value = expert_backward(
        x_and_cot[0], x_and_cot[1], gate_weight[0], up_weight[0], down_weight[0]
    )
    levels = n // 2
    pad = -(-(conv_taps.shape[0] - 1) // 16) * 16
    gated_grad, proj_grad = pl.pallas_call(
        functools.partial(rest_kernel, n),
        out_shape=(shape((tokens_here, quarter), f32), shape((model_width // n, quarter), f32)),
        in_specs=[VMEM] * 5 + [anywhere] * 2 + [VMEM],
        out_specs=(VMEM, VMEM),
        scratch_shapes=[
            pltpu.VMEM((tokens_here, quarter), bf16),
            pltpu.VMEM((n * tokens_here, quarter), bf16),
            pltpu.VMEM((tokens_here, quarter), bf16),
            pltpu.VMEM(out_weight.shape, bf16),
            pltpu.VMEM((2, total_rows, quarter), bf16),
        ]
        + [pltpu.VMEM((total_rows, quarter), bf16)] * 4
        + [
            pltpu.VMEM((tokens_here, model_width), bf16),
            pltpu.VMEM((n, 4, tokens_here // 4, model_width // n), bf16),
            pltpu.VMEM((tokens_here + pad, quarter), f32),
            pltpu.VMEM((2, pad, quarter), bf16),
            pltpu.VMEM((4, 8, tokens_here), f32),
            DMA,
            DMA,
        ]
        + [DMA((2, n))] * 2
        + [DMA((n,))] * 4
        + [DMA((2,))]
        + [DMA((levels,))] * 4
        + [DMA((2 * levels,))] * 2
        + [DMA((3,))] * 2
        + [DMA((n,))] * 2
        + [DMA((3,))] * 4
        + [DMA] * 2,
        compiler_params=params(1),
        name="rest",
    )(partial_value.astype(bf16), squares, conv_out, norm_gain[None, :], select, out_cot, out_weight, conv_taps)
    return (gate_g[None], up_g[None], down_g[None], proj_grad, gated_grad)


def either_plan(*arrays):
    near = lax.axis_size("tp") == 4 and lax.axis_size("sp") == 8
    return near_plan(*arrays) if near else on_device(*arrays)


def solution(mesh):
    placed = (
        P("sp", None),
        P("sp", "tp"),
        P("sp", None),
        P("sp", None),
        P("sp", None),
        P("sp", None, "tp"),
        P("sp", None, "tp"),
        P("sp", "tp", None),
        P("tp", None),
        P("tp"),
        P(None, "tp"),
    )
    return jax.shard_map(
        either_plan,
        mesh=mesh,
        in_specs=placed,
        out_specs=(
            P("sp", None, "tp"),
            P("sp", None, "tp"),
            P("sp", "tp", None),
            P("sp", "tp"),
            P("sp", "tp"),
        ),
        check_vma=False,
    )
```
